32 devices in a mesh: sp: 8 (over z, x), tp: 4 (over y, core).
Axes of the slice: x: 2, y: 2, z: 4, core: 2. Of those that a mesh axis runs over, the one named last changes fastest.
Arguments:
- full_queries: bfloat16 [1024, 1024], P('sp', 'tp'), may hold values from -7 to 7
- full_keys: bfloat16 [1024, 512], P('sp', 'tp'), may hold values from -6 to 6
- full_values: bfloat16 [1024, 512], P('sp', 'tp'), may hold values from -6 to 6
- full_gates: float32 [1024, 8], P(None, 'tp'), may hold values from -512 to 0, as said below
- half_queries: bfloat16 [1024, 1024], P('sp', 'tp'), may hold values from -7 to 7
- half_keys: bfloat16 [1024, 512], P('sp', 'tp'), may hold values from -6 to 6
- half_values: bfloat16 [1024, 512], P('sp', 'tp'), may hold values from -6 to 6
- half_gates: float32 [1024, 16], P(None, 'tp'), may hold values from -512 to 0, as said below
- residual: bfloat16 [1024, 4096], P('sp'), may hold values from -48 to 48
- full_output: bfloat16 [1024, 4096], P('tp'), may hold values from -0.25 to 0.25
- half_output: bfloat16 [1024, 4096], P('tp'), may hold values from -0.25 to 0.25
- norm_gain: float32 [4096], replicated, may hold values from 0.1 to 1.9
- routes: int32 [1024, 4], P('sp'), may hold values from 0 to 7, all different within a row; in each aligned block of 32 rows (0 to 31, 32 to 63, ...) at most 32 rows name the same one
- route_weights: float32 [1024, 4], P('sp'), may hold values from 0.25 to 1.25
- expert_gate: bfloat16 [8, 4096, 512], P('sp', None, 'tp'), may hold values from -0.09375 to 0.09375
- expert_up: bfloat16 [8, 4096, 512], P('sp', None, 'tp'), may hold values from -0.09375 to 0.09375
- expert_down: bfloat16 [8, 512, 4096], P('sp', 'tp'), may hold values from -0.25 to 0.25
- shared_gate: bfloat16 [4096, 512], P(None, 'tp'), may hold values from -0.09375 to 0.09375
- shared_up: bfloat16 [4096, 512], P(None, 'tp'), may hold values from -0.09375 to 0.09375
- shared_down: bfloat16 [512, 4096], P('tp'), may hold values from -0.25 to 0.25
Outputs:
- mixed: bfloat16 [1024, 4096], P(('sp', 'tp'))
The draws below stay inside these ranges and needn't reach their ends.
Inputs may be any that keep to these rules, and one draw needn't show every extreme that they name: `routes`: in each aligned block of 32 rows no expert is named by more than 32 rows; some expert is named by exactly 32 rows in some block. `full_gates`: each column is a running sum of non-positive terms from the first position on. `half_gates`: each column is a running sum of non-positive terms from the first position on.
All inputs are finite; a program needn't handle non-finite values.
Results may differ from the reference program's by a relative error of at most 0.012.
Values may be sent and summed in bfloat16 or wider, within the bound.
A program may use at most 128 MiB of HBM per device.

```python
import math
import jax
import jax.numpy as jnp
import numpy as np
from jax import lax

D = 4096
WH = 8
WD = 128
WK = 4
NH = 16
ND = 64
NK = 8
FE = 512
FS = 512
TOP = 4
TOK_DEV = 128
SEQUENCE_TOKENS = 1024
TQ = 32
EXPERTS = 8
CAP = 32
N_TP = 4


def clipped_normal(seed_key, shape):
    return jnp.clip(jax.random.normal(seed_key, shape, jnp.float32), -6.0, 6.0)


def cumulative_gates(seed_key, total_head_count, slow_count):
    divided_random_keys = jax.random.split(seed_key, 7)
    order_drawn = jax.random.permutation(divided_random_keys[0], total_head_count)
    gradual_heads = (order_drawn < slow_count).astype(jnp.float32)
    slow_rate = jax.random.uniform(divided_random_keys[1], (total_head_count,), jnp.float32, 0.3, 0.8) / SEQUENCE_TOKENS
    fast_rate = jax.random.uniform(divided_random_keys[2], (total_head_count,), jnp.float32, 0.04, 0.1)
    head_rates = gradual_heads * slow_rate + (1.0 - gradual_heads) * fast_rate
    block_factor = jnp.exp(jax.random.uniform(divided_random_keys[3], (SEQUENCE_TOKENS // TOK_DEV, 1), jnp.float32, math.log(0.5), math.log(2.0)))
    block_factor = jnp.repeat(block_factor, TOK_DEV, axis=0)
    roughness = jax.random.uniform(divided_random_keys[4], (SEQUENCE_TOKENS, total_head_count), jnp.float32, 0.3, 1.7)
    logarithm_steps = -head_rates[None, :] * block_factor * roughness
    spike_position = jax.random.randint(divided_random_keys[5], (2,), 0, SEQUENCE_TOKENS)
    spike_penalty = jax.random.uniform(divided_random_keys[6], (2, total_head_count), jnp.float32, 0.2, 0.4)
    sequence_positions = jnp.arange(SEQUENCE_TOKENS)
    for spike_index in range(2):
        spike_row = (sequence_positions == spike_position[spike_index]).astype(jnp.float32)[:, None]
        logarithm_steps = logarithm_steps + spike_row * jnp.log(1.0 - spike_penalty[spike_index])[None, :] * gradual_heads[None, :]
    return jnp.cumsum(logarithm_steps, axis=0)


def draw_full_queries(key, part):
    drawn = clipped_normal(jax.random.fold_in(key, 1), (SEQUENCE_TOKENS, WH * WD))
    return drawn.astype(jnp.bfloat16)


def draw_full_keys(key, part):
    drawn = clipped_normal(jax.random.fold_in(key, 2), (SEQUENCE_TOKENS, WK * WD))
    return drawn.astype(jnp.bfloat16)


def draw_half_queries(key, part):
    drawn = clipped_normal(jax.random.fold_in(key, 3), (SEQUENCE_TOKENS, NH * ND))
    return drawn.astype(jnp.bfloat16)


def draw_half_keys(key, part):
    drawn = clipped_normal(jax.random.fold_in(key, 4), (SEQUENCE_TOKENS, NK * ND))
    return drawn.astype(jnp.bfloat16)


def draw_full_gates(key, part):
    slow_count = WH // 2
    return cumulative_gates(jax.random.fold_in(key, 5), WH, slow_count).astype(jnp.float32)


def draw_half_gates(key, part):
    slow_count = NH // 2
    return cumulative_gates(jax.random.fold_in(key, 6), NH, slow_count).astype(jnp.float32)


def draw_residual(key, part):
    divided_random_keys = jax.random.split(jax.random.fold_in(key, 7), 3)
    drawn = clipped_normal(divided_random_keys[0], (SEQUENCE_TOKENS, D))
    row_scale = jnp.exp(jax.random.uniform(divided_random_keys[1], (SEQUENCE_TOKENS, 1), jnp.float32, math.log(0.5), math.log(2.0)))
    column_scale = jnp.exp(jax.random.uniform(divided_random_keys[2], (1, D), jnp.float32, math.log(0.4), math.log(4.0)))
    return (drawn * row_scale * column_scale).astype(jnp.bfloat16)


def steps_of(stream_key, shape, shards, smallest, top_value):
    level = 1.0
    for position, blocks in shards:
        heights = jax.random.uniform(jax.random.fold_in(jax.random.fold_in(stream_key, 6), position), (blocks,), jnp.float32, smallest / len(shards), top_value / len(shards))
        level = level * jnp.repeat(jnp.exp(heights), shape[position] // blocks).reshape((-1,) + (1,) * (len(shape) - 1 - position))
    return level


def deal_out(key, own, number, rows, count, top, limit, lean):
    ranking = jax.random.permutation(key, count)
    heavy_load, usual = portions_of(count, rows * top, limit, lean, True), portions_of(count, rows * top, limit, lean, False)
    places = jnp.arange(count)

    def named(sizes, turn):
        used = int((sizes > 0).sum())
        fixed = max(1, used // 4)
        shifted = fixed + (places - fixed + turn * (used - fixed)) % max(1, count - fixed)
        return jnp.zeros((count,), jnp.int32).at[ranking[jnp.where(places < fixed, places, shifted)]].set(jnp.asarray(sizes, jnp.int32))

    sizes = jnp.where(number % 4 == 0, named(heavy_load, number // 4), named(usual, number - number // 4 - 1))
    mixed = jax.random.permutation(jax.random.fold_in(own, 3), count)
    source_of, sink = mixed[0:count // 2 * 2:2], mixed[1:count // 2 * 2:2]
    margin = jnp.minimum(sizes[source_of] - 1, limit - sizes[sink]) // 2
    margin = jnp.where((source_of == ranking[0]) | (sink == ranking[0]) | (sizes[sink] == 0), 0, jnp.maximum(margin, 0))
    shifted = jax.random.randint(jax.random.fold_in(own, 4), (count // 2,), 0, 1 << 20) % (margin + 1)
    sizes = sizes.at[source_of].add(-shifted).at[sink].add(shifted)
    items = jnp.searchsorted(jnp.cumsum(sizes), jnp.arange(rows * top), side="right").astype(jnp.int32)
    listing = items.reshape(top, rows).T
    listing = listing[jax.random.permutation(jax.random.fold_in(own, 1), rows)]
    turn = jax.random.randint(jax.random.fold_in(own, 2), (rows, 1), 0, top)
    return jnp.take_along_axis(listing, (jnp.arange(top)[None, :] + turn) % top, axis=1)


def portions_of(number_of, total, limit, skew, full):
    portions = [(1 << 20) // math.isqrt(grade ** skew) + 1 for grade in range(1, number_of + 1)]
    largest = limit if full else min(limit, max(-(-total // number_of), total * portions[0] // sum(portions)))
    least = 1 if total - largest >= number_of - 1 else 0
    given, surplus = [largest] + [least] * (number_of - 1), total - largest - least * (number_of - 1)
    while surplus > 0:
        movable = [i for i in range(1, number_of) if given[i] < largest] or [i for i in range(1, number_of) if given[i] < limit]
        pool, left = sum([portions[i] for i in movable]), surplus
        for i in movable:
            extra = min(limit - given[i], max(1, left * portions[i] // pool), surplus)
            given[i] = given[i] + extra
            surplus = surplus - extra
    return np.array(given)


def normal_values(stream_key, shape, scale, reach, cuts=(), held_as=jnp.bfloat16):
    values = scale * jax.random.normal(stream_key, shape, jnp.float32)
    if cuts:
        values = values * steps_of(stream_key, shape, cuts, -0.22, 0.18)
    return jnp.clip(values, -reach, reach).astype(held_as)


def setup_inputs(seed: int = 0) -> dict:
    streams_of = jax.random.split(jax.random.key(seed), 21)
    full_queries = draw_full_queries(jax.random.fold_in(streams_of[20], 71), 0)
    full_keys = draw_full_keys(jax.random.fold_in(streams_of[20], 71), 0)
    full_values = normal_values(streams_of[2], (SEQUENCE_TOKENS, WK * WD), 1.0, 6.0, ((0, 8), (1, 4)))
    full_gates = draw_full_gates(jax.random.fold_in(streams_of[20], 71), 0)
    half_queries = draw_half_queries(jax.random.fold_in(streams_of[20], 71), 0)
    half_keys = draw_half_keys(jax.random.fold_in(streams_of[20], 71), 0)
    half_values = normal_values(streams_of[6], (SEQUENCE_TOKENS, NK * ND), 1.0, 6.0, ((0, 8), (1, 4)))
    half_gates = draw_half_gates(jax.random.fold_in(streams_of[20], 71), 0)
    residual = draw_residual(jax.random.fold_in(streams_of[20], 71), 0)
    full_output = normal_values(streams_of[9], (WH * WD, D), ((WH * WD + NH * ND) // 4) ** -0.5, 0.25, ((0, 4),))
    half_output = normal_values(streams_of[10], (NH * ND, D), ((WH * WD + NH * ND) // 4) ** -0.5, 0.25, ((0, 4),))
    norm_gain = jnp.clip(1.0 + 0.18 * jax.random.normal(streams_of[11], (D,), jnp.float32), 0.1, 1.9)
    routes_keys = jax.random.split(jax.random.fold_in(streams_of[12], 1), SEQUENCE_TOKENS // TQ)
    routes_turns = jax.random.permutation(jax.random.fold_in(streams_of[12], 3), SEQUENCE_TOKENS // TQ)
    routes = jax.vmap(lambda own, number: deal_out(jax.random.fold_in(streams_of[12], 2), own, number, TQ, EXPERTS, TOP, CAP, 2))(routes_keys, routes_turns).reshape((SEQUENCE_TOKENS, TOP))
    route_weights = jnp.clip(0.25 + 1.0 * jax.random.uniform(streams_of[13], (SEQUENCE_TOKENS, TOP), jnp.float32) ** steps_of(streams_of[13], (SEQUENCE_TOKENS, TOP), ((0, 8),), -0.2, 0.2), 0.25, 1.25)
    expert_gate = normal_values(streams_of[14], (EXPERTS, D, FE), D ** -0.5, 0.09375, ((0, 8), (2, 4)))
    expert_up = normal_values(streams_of[15], (EXPERTS, D, FE), D ** -0.5, 0.09375, ((0, 8), (2, 4)))
    expert_down = normal_values(streams_of[16], (EXPERTS, FE, D), FE ** -0.5, 0.25, ((0, 8), (1, 4)))
    shared_gate = normal_values(streams_of[17], (D, FS), D ** -0.5, 0.09375, ((1, 4),))
    shared_up = normal_values(streams_of[18], (D, FS), D ** -0.5, 0.09375, ((1, 4),))
    shared_down = normal_values(streams_of[19], (FS, D), FS ** -0.5, 0.25, ((0, 4),))
    return dict(full_queries=full_queries, full_keys=full_keys, full_values=full_values, full_gates=full_gates, half_queries=half_queries, half_keys=half_keys, half_values=half_values, half_gates=half_gates, residual=residual, full_output=full_output, half_output=half_output, norm_gain=norm_gain, routes=routes, route_weights=route_weights, expert_gate=expert_gate, expert_up=expert_up, expert_down=expert_down, shared_gate=shared_gate, shared_up=shared_up, shared_down=shared_down)


def group_attention(queries, keys_in, values_in, gates, total_head_count, key_heads, head_dim):
    tokens = queries.shape[0]
    group_size = total_head_count // key_heads
    block_rows = math.gcd(tokens, 256)
    key_float = keys_in.astype(jnp.float32).reshape(tokens, key_heads, head_dim)
    value_float = values_in.astype(jnp.float32).reshape(tokens, key_heads, head_dim)
    key_gates = jnp.transpose(gates.reshape(tokens, key_heads, group_size), (1, 2, 0))[:, :, None, :]
    sequence_positions = jnp.arange(tokens, dtype=jnp.int32)

    def one_block(block_index):
        first_row = (block_index * block_rows).astype(jnp.int32)
        query_rows = lax.dynamic_slice_in_dim(queries, first_row, block_rows, 0)
        query_rows = query_rows.astype(jnp.float32).reshape(block_rows, key_heads, group_size, head_dim)
        query_gates = lax.dynamic_slice_in_dim(gates, first_row, block_rows, 0)
        query_gates = jnp.transpose(query_gates.reshape(block_rows, key_heads, group_size), (1, 2, 0))[..., None]
        scores = jnp.einsum('tkgd,skd->kgts', query_rows, key_float) * head_dim ** (-0.5)
        scores = scores + query_gates - key_gates
        query_pos = first_row + jnp.arange(block_rows, dtype=jnp.int32)
        allowed = sequence_positions[None, :] <= query_pos[:, None]
        scores = jnp.where(allowed, scores, -jnp.inf)
        row_max = lax.optimization_barrier(jnp.max(scores, axis=-1, keepdims=True))
        weights = jnp.where(allowed, jnp.exp(scores - row_max), 0.0)
        row_total = lax.optimization_barrier(jnp.sum(weights, axis=-1))
        rounded = lax.optimization_barrier(weights.astype(jnp.bfloat16)).astype(jnp.float32)
        summed = jnp.einsum('kgts,skd->kgtd', rounded, value_float)
        result = summed / row_total[..., None]
        result = jnp.transpose(result, (2, 0, 1, 3)).reshape(block_rows, total_head_count * head_dim)
        return result.astype(jnp.bfloat16)
    pieces = lax.map(one_block, jnp.arange(tokens // block_rows, dtype=jnp.int32))
    return pieces.reshape(tokens, total_head_count * head_dim)

def block_swiglu(rows_in, gate_weight, up_weight, down_weight):
    gate_part = jnp.dot(rows_in, gate_weight, preferred_element_type=jnp.float32)
    up_part = jnp.dot(rows_in, up_weight, preferred_element_type=jnp.float32)
    hidden = (jax.nn.silu(gate_part) * up_part).astype(jnp.bfloat16)
    block_width = hidden.shape[1] // N_TP
    summed = jnp.zeros((rows_in.shape[0], down_weight.shape[1]), jnp.float32)
    for block_index in range(N_TP):
        low_edge = block_index * block_width
        product = jnp.dot(hidden[:, low_edge:low_edge + block_width], down_weight[low_edge:low_edge + block_width], preferred_element_type=jnp.float32)
        summed = summed + lax.optimization_barrier(product.astype(jnp.bfloat16)).astype(jnp.float32)
    return summed

def reference(full_queries, full_keys, full_values, full_gates, half_queries, half_keys, half_values, half_gates, residual, full_output, half_output, norm_gain, routes, route_weights, expert_gate, expert_up, expert_down, shared_gate, shared_up, shared_down):
    full_attention = group_attention(full_queries, full_keys, full_values, full_gates, WH, WK, WD)
    half_attention = group_attention(half_queries, half_keys, half_values, half_gates, NH, NK, ND)
    middle = residual.astype(jnp.float32) + jnp.dot(full_attention, full_output, preferred_element_type=jnp.float32) + jnp.dot(half_attention, half_output, preferred_element_type=jnp.float32)
    normed = (middle * lax.rsqrt(lax.optimization_barrier(jnp.mean(middle * middle, axis=-1, keepdims=True)) + 1e-06) * norm_gain).astype(jnp.bfloat16)
    shared_out = block_swiglu(normed, shared_gate, shared_up, shared_down)
    flat_routes = routes.reshape(-1).astype(jnp.int32)
    flat_weights = route_weights.reshape(-1)
    slot_total = SEQUENCE_TOKENS // TQ * CAP

    def one_expert(routed_sum, expert_index):
        sort_key = jnp.where(flat_routes == expert_index, 0, 1).astype(jnp.int32)
        route_order = jnp.argsort(sort_key, stable=True)[:slot_total].astype(jnp.int32)
        is_valid = (flat_routes[route_order] == expert_index).astype(jnp.float32)
        token_index = (route_order // TOP).astype(jnp.int32)
        expert_rows = normed[token_index]
        result = block_swiglu(expert_rows, expert_gate[expert_index], expert_up[expert_index], expert_down[expert_index])
        result = lax.optimization_barrier(result.astype(jnp.bfloat16)).astype(jnp.float32)
        route_scale = flat_weights[route_order] * is_valid
        return (routed_sum.at[token_index].add(route_scale[:, None] * result), None)
    routed, _ = lax.scan(one_expert, jnp.zeros((SEQUENCE_TOKENS, D), jnp.float32), jnp.arange(EXPERTS, dtype=jnp.int32))
    return (middle + shared_out + routed).astype(jnp.bfloat16)
```

```python
import functools

import jax
import jax.numpy as jnp
from jax import lax
from jax.experimental import pallas as pl
from jax.experimental.pallas import tpu as pltpu
from jax.sharding import PartitionSpec as P

D = 4096
WD = 128
ND = 64
TOP = 4


def group_setup(queries, gates, offset, key_heads, head_dim):
    row_count = queries.shape[0]
    group_size = queries.shape[1] // head_dim // key_heads
    shaped = queries.reshape(row_count, key_heads, group_size, head_dim)
    own_gates = lax.dynamic_slice_in_dim(gates, offset, row_count, 0)
    query_gates = jnp.transpose(own_gates.reshape(row_count, key_heads, group_size), (1, 2, 0))[
        ..., None
    ]
    return (shaped, query_gates)


def empty_state(shaped):
    row_count, key_heads, group_size, head_dim = shaped.shape
    return (
        jnp.full((key_heads, group_size, row_count), -1e30, jnp.float32),
        jnp.zeros((key_heads, group_size, row_count), jnp.float32),
        jnp.zeros((key_heads, group_size, row_count, head_dim), jnp.float32),
    )


def group_update(
    running, shaped, query_gates, all_gates, key_rows, value_rows, span_start, query_pos, head_dim
):
    row_max, row_total, weighted = running
    key_count = key_rows.shape[0]
    key_heads = shaped.shape[1]
    group_size = shaped.shape[2]
    key_shaped = key_rows.reshape(key_count, key_heads, head_dim)
    value_shaped = value_rows.reshape(key_count, key_heads, head_dim)
    key_gates = lax.dynamic_slice_in_dim(all_gates, span_start, key_count, 0)
    key_gates = jnp.transpose(key_gates.reshape(key_count, key_heads, group_size), (1, 2, 0))[
        :, :, None, :
    ]
    scores = jnp.einsum("tkgd,skd->kgts", shaped, key_shaped, preferred_element_type=jnp.float32)
    scores = scores * head_dim ** (-0.5) + query_gates - key_gates
    key_pos = span_start + jnp.arange(key_count, dtype=jnp.int32)
    allowed = key_pos[None, :] <= query_pos[:, None]
    masked = jnp.where(allowed, scores, -1e30)
    new_max = jnp.maximum(row_max, jnp.max(masked, axis=-1))
    weights = jnp.where(allowed, jnp.exp(masked - new_max[..., None]), 0.0)
    shrink = jnp.exp(row_max - new_max)
    new_total = row_total * shrink + jnp.sum(weights, axis=-1)
    new_weighted = weighted * shrink[..., None] + jnp.einsum(
        "kgts,skd->kgtd",
        weights.astype(jnp.bfloat16),
        value_shaped,
        preferred_element_type=jnp.float32,
    )
    return (new_max, new_total, new_weighted)


def group_finish(running):
    weighted = running[2] / running[1][..., None]
    row_count = weighted.shape[2]
    return jnp.transpose(weighted, (2, 0, 1, 3)).reshape(row_count, -1).astype(jnp.bfloat16)


def span_for(key_count):
    if key_count <= 2048:
        return key_count
    return max((candidate for candidate in range(1, 2049) if key_count % candidate == 0))


def build_picks(route_rows, experts_count, capacity):
    flat_routes = route_rows.reshape(-1)
    onehot = (flat_routes[:, None] == jnp.arange(experts_count, dtype=jnp.int32)[None, :]).astype(
        jnp.int32
    )
    earlier = jnp.cumsum(onehot, axis=0) - onehot
    slot_rank = jnp.sum(earlier * onehot, axis=1)
    slot_ids = flat_routes * capacity + slot_rank
    picked = slot_ids[:, None] == jnp.arange(experts_count * capacity, dtype=jnp.int32)[None, :]
    return picked.astype(jnp.bfloat16).reshape(
        route_rows.shape[0], route_rows.shape[1], experts_count * capacity
    )


def fill_slots(picked, token_rows):
    occupancy = jnp.sum(picked, axis=1)
    return jnp.einsum(
        "ts,td->sd", occupancy, token_rows, preferred_element_type=jnp.float32
    ).astype(jnp.bfloat16)


MESH_IDS = pl.DeviceIdType.MESH
WHOLE_VMEM = pl.BlockSpec(memory_space=pltpu.VMEM)


def flipped(index, bits):
    result = index
    bit = 1
    while bit <= bits:
        if bits & bit:
            result = result + bit * (1 - 2 * ((index // bit) % 2))
        bit *= 2
    return result


def remote(source, target, send_sem, recv_sem, device):
    return pltpu.make_async_remote_copy(
        src_ref=source,
        dst_ref=target,
        send_sem=send_sem,
        recv_sem=recv_sem,
        device_id=device,
        device_id_type=MESH_IDS,
    )


def greet(devices):
    barrier = pltpu.get_barrier_semaphore()
    for device in devices:
        pl.semaphore_signal(barrier, inc=1, device_id=device, device_id_type=MESH_IDS)
    pl.semaphore_wait(barrier, len(devices))


def sp_peers(members):
    own = lax.axis_index("sp")
    pair, outer = own % 2, own // 2
    partner = {"sp": outer * 2 + 1 - pair}
    others = [{"sp": flipped(outer, d) * 2 + pair} for d in range(1, members // 2)]
    return own, pair, outer, partner, others


def gather_kernel(members, quarters, with_tp, *refs):
    if with_tp:
        x_ref, o_ref, t_ref = refs[:3]
        send_z, recv_z, send_x, recv_x, send_t, recv_t = refs[3:]
    else:
        x_ref, o_ref = refs[:2]
        send_z, recv_z, send_x, recv_x = refs[2:]
    half = members // 2
    own, pair, outer, partner, others = sp_peers(members)
    tp = lax.axis_index("tp")
    mates = [{"tp": flipped(tp, d)} for d in range(1, quarters)] if with_tp else []
    greet([partner] + others + mates)
    started = []
    for d in range(1, half):
        started.append(
            remote(x_ref, o_ref.at[own], send_z.at[d], recv_z.at[d], others[d - 1])
        )
    started.append(remote(x_ref, o_ref.at[own], send_x.at[0], recv_x.at[0], partner))
    for d in range(1, len(mates) + 1):
        started.append(remote(x_ref, t_ref.at[tp], send_t.at[d], recv_t.at[d], mates[d - 1]))
    for copy in started:
        copy.start()
    o_ref[own] = x_ref[...]
    if with_tp:
        t_ref[tp] = x_ref[...]
    passed = []
    for d in range(1, half):
        started[d - 1].wait_recv()
        block = flipped(outer, d) * 2 + pair
        copy = remote(o_ref.at[block], o_ref.at[block], send_x.at[d], recv_x.at[d], partner)
        copy.start()
        passed.append(copy)
    for copy in started[half - 1 :] + passed:
        copy.wait_recv()
    for copy in started + passed:
        copy.wait_send()


def gather_rows(block, collective_id, with_tp):
    members, quarters = lax.axis_size("sp"), lax.axis_size("tp")
    half = members // 2
    outs = [jax.ShapeDtypeStruct((members,) + block.shape, block.dtype)]
    sems = [pltpu.SemaphoreType.DMA((half,))] * 4
    if with_tp:
        outs.append(jax.ShapeDtypeStruct((quarters,) + block.shape, block.dtype))
        sems = sems + [pltpu.SemaphoreType.DMA((quarters,))] * 2
    return pl.pallas_call(
        functools.partial(gather_kernel, members, quarters, with_tp),
        out_shape=tuple(outs),
        in_specs=[WHOLE_VMEM],
        out_specs=tuple([WHOLE_VMEM] * len(outs)),
        scratch_shapes=sems,
        compiler_params=pltpu.CompilerParams(collective_id=collective_id, has_side_effects=True),
        cost_estimate=pl.CostEstimate(flops=0, bytes_accessed=50000000, transcendentals=0),
    )(block)


def add_norm_kernel(
    quarters, parts_ref, residual_ref, gain_ref, middle_ref, normed_ref, landed, send, recv
):
    tp = lax.axis_index("tp")
    mates = [{"tp": flipped(tp, d)} for d in range(1, quarters)]
    greet(mates)
    copies = [
        remote(
            parts_ref.at[flipped(tp, d)], landed.at[d - 1], send.at[d], recv.at[d], mates[d - 1]
        )
        for d in range(1, quarters)
    ]
    for copy in copies:
        copy.start()
    middle = parts_ref[tp].astype(jnp.float32) + residual_ref[...].astype(jnp.float32)
    for d, copy in enumerate(copies):
        copy.wait_recv()
        middle = middle + landed[d].astype(jnp.float32)
    middle_ref[...] = middle
    scale = lax.rsqrt(jnp.mean(middle * middle, axis=-1, keepdims=True) + 1e-06)
    normed_ref[...] = (middle * scale * gain_ref[...]).astype(jnp.bfloat16)
    for copy in copies:
        copy.wait_send()


def add_norm(parts, residual, gain):
    quarters, rows, width = parts.shape
    return pl.pallas_call(
        functools.partial(add_norm_kernel, quarters),
        out_shape=(
            jax.ShapeDtypeStruct((rows, width), jnp.float32),
            jax.ShapeDtypeStruct((rows, width), jnp.bfloat16),
        ),
        in_specs=[WHOLE_VMEM] * 3,
        out_specs=(WHOLE_VMEM, WHOLE_VMEM),
        scratch_shapes=[
            pltpu.VMEM((quarters - 1, rows, width), jnp.bfloat16),
            pltpu.SemaphoreType.DMA((quarters,)),
            pltpu.SemaphoreType.DMA((quarters,)),
        ],
        compiler_params=pltpu.CompilerParams(collective_id=2, has_side_effects=True),
        cost_estimate=pl.CostEstimate(flops=0, bytes_accessed=40000000, transcendentals=0),
    )(parts, residual, gain)


def return_kernel(
    members,
    quarters,
    routed_ref,
    shared_ref,
    middle_ref,
    out_ref,
    from_x,
    staged,
    from_z,
    from_t,
    send_x,
    recv_x,
    send_z,
    recv_z,
    send_t,
    recv_t,
):
    half = members // 2
    own, pair, outer, partner, others = sp_peers(members)
    tp = lax.axis_index("tp")
    mates = [{"tp": flipped(tp, d)} for d in range(1, quarters)]
    greet([partner] + others + mates)
    to_x = [
        remote(
            routed_ref.at[flipped(outer, d) * 2 + 1 - pair],
            from_x.at[d],
            send_x.at[d],
            recv_x.at[d],
            partner,
        )
        for d in range(half)
    ]
    for d in list(range(1, half))[::-1] + [0]:
        to_x[d].start()
    to_t = [
        remote(
            shared_ref.at[flipped(tp, d)], from_t.at[d - 1], send_t.at[d], recv_t.at[d], mates[d - 1]
        )
        for d in range(1, quarters)
    ]
    for copy in to_t:
        copy.start()
    to_z = [
        remote(staged.at[d], from_z.at[d], send_z.at[d], recv_z.at[d], others[d - 1])
        for d in range(1, half)
    ]
    for d in range(1, half)[::-1]:
        to_x[d].wait_recv()
        staged[d] = (
            routed_ref[flipped(outer, d) * 2 + pair].astype(jnp.float32)
            + from_x[d].astype(jnp.float32)
        ).astype(jnp.bfloat16)
        to_z[d - 1].start()
    total = middle_ref[...] + shared_ref[tp].astype(jnp.float32)
    for d, copy in enumerate(to_t):
        copy.wait_recv()
        total = total + from_t[d].astype(jnp.float32)
    to_x[0].wait_recv()
    total = total + routed_ref[own].astype(jnp.float32) + from_x[0].astype(jnp.float32)
    for d in range(1, half):
        to_z[d - 1].wait_recv()
        total = total + from_z[d].astype(jnp.float32)
    out_ref[...] = total.astype(jnp.bfloat16)
    for copy in to_x + to_t + to_z:
        copy.wait_send()


def return_rows(routed, shared, middle):
    members, rows, width = routed.shape
    quarters = shared.shape[0]
    half = members // 2
    sems = [pltpu.SemaphoreType.DMA((half,))] * 4 + [pltpu.SemaphoreType.DMA((quarters,))] * 2
    return pl.pallas_call(
        functools.partial(return_kernel, members, quarters),
        out_shape=jax.ShapeDtypeStruct((rows, width), jnp.bfloat16),
        in_specs=[WHOLE_VMEM] * 3,
        out_specs=WHOLE_VMEM,
        scratch_shapes=[
            pltpu.VMEM((half, rows, width), jnp.bfloat16),
            pltpu.VMEM((half, rows, width), jnp.bfloat16),
            pltpu.VMEM((half, rows, width), jnp.bfloat16),
            pltpu.VMEM((quarters - 1, rows, width), jnp.bfloat16),
        ]
        + sems,
        compiler_params=pltpu.CompilerParams(collective_id=4, has_side_effects=True),
        cost_estimate=pl.CostEstimate(flops=0, bytes_accessed=80000000, transcendentals=0),
    )(routed, shared, middle)


def tp_blocks(own):
    quarters = lax.axis_size("tp")
    blocks = [own]
    bit = quarters // 2
    while bit:
        pairs = [(j, j ^ bit) for j in range(quarters)]
        blocks = blocks + [lax.ppermute(block, "tp", pairs) for block in blocks]
        bit //= 2
    return blocks


def body(
    full_queries,
    full_keys,
    full_values,
    full_gates,
    half_queries,
    half_keys,
    half_values,
    half_gates,
    residual,
    full_output,
    half_output,
    norm_gain,
    routes,
    route_weights,
    expert_gate,
    expert_up,
    expert_down,
    shared_gate,
    shared_up,
    shared_down,
):
    row_count = full_queries.shape[0]
    quarters = lax.axis_size("tp")
    quarter = lax.axis_index("tp")
    quarter_rows = row_count // quarters
    experts_count = lax.axis_size("sp")
    own_expert = lax.axis_index("sp")
    capacity = 2 * quarter_rows * TOP // experts_count
    gate_blocks = tp_blocks(expert_gate[0])
    up_blocks = tp_blocks(expert_up[0])
    down_blocks = tp_blocks(expert_down[0])
    offset = own_expert * row_count
    query_pos = offset + jnp.arange(row_count, dtype=jnp.int32)
    dense_routes = capacity >= quarter_rows
    columns = [full_keys, full_values, half_keys, half_values]
    widths = [column.shape[1] for column in columns]
    if dense_routes:
        chosen = routes[:, :, None] == jnp.arange(experts_count, dtype=jnp.int32)
        scales = jnp.sum(jnp.where(chosen, route_weights[:, :, None], 0.0), axis=1)
        high = lax.reduce_precision(scales, 8, 7)
        rest = lax.reduce_precision(scales - high, 8, 7)
        low = lax.reduce_precision(scales - high - rest, 8, 7)
        thirds = jnp.concatenate([high, rest, low], axis=1).astype(jnp.bfloat16)
        padded = -(-thirds.shape[1] // 128) * 128
        columns.append(jnp.pad(thirds, ((0, 0), (0, padded - thirds.shape[1]))))
    gathered_rows = gather_rows(jnp.concatenate(columns, axis=1), 1, False)[0]
    key_count = experts_count * row_count
    flat_gathered = gathered_rows.reshape(key_count, -1)
    members = []
    low_edge = 0
    for width in widths:
        members.append(flat_gathered[:, low_edge : low_edge + width])
        low_edge += width
    full_shaped, full_query_gates = group_setup(
        full_queries, full_gates, offset, full_keys.shape[1] // WD, WD
    )
    half_shaped, half_query_gates = group_setup(
        half_queries, half_gates, offset, half_keys.shape[1] // ND, ND
    )
    initial = empty_state(full_shaped) + empty_state(half_shaped)
    span_rows = span_for(key_count)

    def one_span(running, span_index):
        span_start = span_index * span_rows
        sliced = tuple(
            (lax.dynamic_slice_in_dim(member, span_start, span_rows, 0) for member in members)
        )

        def update(current):
            full_new = group_update(
                current[:3],
                full_shaped,
                full_query_gates,
                full_gates,
                sliced[0],
                sliced[1],
                span_start,
                query_pos,
                WD,
            )
            half_new = group_update(
                current[3:],
                half_shaped,
                half_query_gates,
                half_gates,
                sliced[2],
                sliced[3],
                span_start,
                query_pos,
                ND,
            )
            return full_new + half_new

        if key_count == span_rows:
            return update(running), None
        last_row = offset + row_count - 1
        return (
            lax.cond(span_start <= last_row, update, lambda unchanged: unchanged, running),
            None,
        )

    if key_count == span_rows:
        result, _ = one_span(initial, 0)
    else:
        result, _ = lax.scan(one_span, initial, jnp.arange(key_count // span_rows, dtype=jnp.int32))
    full_attention = group_finish(result[:3])
    half_attention = group_finish(result[3:])
    partial_out = jnp.dot(
        full_attention, full_output, preferred_element_type=jnp.float32
    ) + jnp.dot(half_attention, half_output, preferred_element_type=jnp.float32)
    own_residual = lax.dynamic_slice_in_dim(residual, quarter * quarter_rows, quarter_rows, 0)
    own_middle, own_normed = add_norm(
        partial_out.astype(jnp.bfloat16).reshape(quarters, quarter_rows, D),
        own_residual,
        norm_gain.reshape(1, D),
    )
    if dense_routes:
        expert_rows, normed = gather_rows(own_normed, 3, True)
        flat_rows = expert_rows.reshape(-1, D)
    else:
        normed = lax.all_gather(own_normed, "tp", axis=0, tiled=True)
        own_routes = lax.dynamic_slice_in_dim(routes, quarter * quarter_rows, quarter_rows, 0)
        own_picks = build_picks(own_routes, experts_count, capacity)
        buffer_rows = fill_slots(own_picks, own_normed).reshape(experts_count, capacity, D)
        received = lax.all_to_all(buffer_rows, "sp", split_axis=0, concat_axis=0, tiled=True)
        flat_rows = received.reshape(-1, D)
    normed = normed.reshape(row_count, D)
    shared_hidden = (
        jax.nn.silu(jnp.dot(normed, shared_gate, preferred_element_type=jnp.float32))
        * jnp.dot(normed, shared_up, preferred_element_type=jnp.float32)
    ).astype(jnp.bfloat16)
    shared_term = (
        jnp.dot(shared_hidden, shared_down, preferred_element_type=jnp.float32)
        .astype(jnp.bfloat16)
        .reshape(quarters, quarter_rows, D)
    )
    total = jnp.zeros((flat_rows.shape[0], D), jnp.float32)
    for gate_block, up_block, down_block in zip(gate_blocks, up_blocks, down_blocks):
        hidden = (
            jax.nn.silu(jnp.dot(flat_rows, gate_block, preferred_element_type=jnp.float32))
            * jnp.dot(flat_rows, up_block, preferred_element_type=jnp.float32)
        ).astype(jnp.bfloat16)
        total = total + jnp.dot(hidden, down_block, preferred_element_type=jnp.float32)
    if dense_routes:
        thirds = gathered_rows[:, :, low_edge : low_edge + 3 * experts_count].astype(jnp.float32)
        thirds = lax.dynamic_slice_in_dim(thirds, quarter * quarter_rows, quarter_rows, 1)
        mine = jnp.arange(3 * experts_count, dtype=jnp.int32) % experts_count == own_expert
        row_scales = jnp.sum(jnp.where(mine, thirds, 0.0), axis=2).reshape(-1, 1)
        routed = (total * row_scales).astype(jnp.bfloat16)
        return return_rows(
            routed.reshape(experts_count, quarter_rows, D), shared_term, own_middle
        )
    finished_rows = total.astype(jnp.bfloat16).reshape(received.shape)
    summed = lax.psum_scatter(shared_term, "tp", scatter_dimension=0, tiled=True).astype(
        jnp.float32
    )[0]
    returned = lax.all_to_all(finished_rows, "sp", split_axis=0, concat_axis=0, tiled=True)
    gathered = jnp.einsum(
        "tks,sd->tkd",
        own_picks,
        returned.reshape(experts_count * capacity, D),
        preferred_element_type=jnp.float32,
    )
    own_weights = lax.dynamic_slice_in_dim(route_weights, quarter * quarter_rows, quarter_rows, 0)
    routed = jnp.sum(own_weights[..., None] * gathered, axis=1)
    return (own_middle + summed + routed).astype(jnp.bfloat16)


def solution(mesh):
    return jax.shard_map(
        body,
        mesh=mesh,
        in_specs=(
            P("sp", "tp"),
            P("sp", "tp"),
            P("sp", "tp"),
            P(None, "tp"),
            P("sp", "tp"),
            P("sp", "tp"),
            P("sp", "tp"),
            P(None, "tp"),
            P("sp", None),
            P("tp", None),
            P("tp", None),
            P(),
            P("sp", None),
            P("sp", None),
            P("sp", None, "tp"),
            P("sp", None, "tp"),
            P("sp", "tp", None),
            P(None, "tp"),
            P(None, "tp"),
            P("tp", None),
        ),
        out_specs=P(("sp", "tp"), None),
        check_vma=False,
    )
```

```python
import functools

import jax
import jax.numpy as jnp
from jax import lax
from jax.experimental import pallas as pl
from jax.experimental.pallas import tpu as pltpu
from jax.sharding import PartitionSpec as P

D = 4096
WD = 128
ND = 64
TOP = 4


def group_setup(queries, gates, offset, key_heads, head_dim):
    row_count = queries.shape[0]
    group_size = queries.shape[1] // head_dim // key_heads
    shaped = queries.reshape(row_count, key_heads, group_size, head_dim)
    own_gates = lax.dynamic_slice_in_dim(gates, offset, row_count, 0)
    query_gates = jnp.transpose(own_gates.reshape(row_count, key_heads, group_size), (1, 2, 0))[
        ..., None
    ]
    return (shaped, query_gates)


def empty_state(shaped):
    row_count, key_heads, group_size, head_dim = shaped.shape
    return (
        jnp.full((key_heads, group_size, row_count), -1e30, jnp.float32),
        jnp.zeros((key_heads, group_size, row_count), jnp.float32),
        jnp.zeros((key_heads, group_size, row_count, head_dim), jnp.float32),
    )


def group_update(
    running, shaped, query_gates, all_gates, key_rows, value_rows, span_start, query_pos, head_dim
):
    row_max, row_total, weighted = running
    key_count = key_rows.shape[0]
    key_heads = shaped.shape[1]
    group_size = shaped.shape[2]
    key_shaped = key_rows.reshape(key_count, key_heads, head_dim)
    value_shaped = value_rows.reshape(key_count, key_heads, head_dim)
    key_gates = lax.dynamic_slice_in_dim(all_gates, span_start, key_count, 0)
    key_gates = jnp.transpose(key_gates.reshape(key_count, key_heads, group_size), (1, 2, 0))[
        :, :, None, :
    ]
    scores = jnp.einsum("tkgd,skd->kgts", shaped, key_shaped, preferred_element_type=jnp.float32)
    scores = scores * head_dim ** (-0.5) + query_gates - key_gates
    key_pos = span_start + jnp.arange(key_count, dtype=jnp.int32)
    allowed = key_pos[None, :] <= query_pos[:, None]
    masked = jnp.where(allowed, scores, -1e30)
    new_max = jnp.maximum(row_max, jnp.max(masked, axis=-1))
    weights = jnp.where(allowed, jnp.exp(masked - new_max[..., None]), 0.0)
    shrink = jnp.exp(row_max - new_max)
    new_total = row_total * shrink + jnp.sum(weights, axis=-1)
    new_weighted = weighted * shrink[..., None] + jnp.einsum(
        "kgts,skd->kgtd",
        weights.astype(jnp.bfloat16),
        value_shaped,
        preferred_element_type=jnp.float32,
    )
    return (new_max, new_total, new_weighted)


def group_finish(running):
    weighted = running[2] / running[1][..., None]
    row_count = weighted.shape[2]
    return jnp.transpose(weighted, (2, 0, 1, 3)).reshape(row_count, -1).astype(jnp.bfloat16)


def span_for(key_count):
    if key_count <= 2048:
        return key_count
    return max((candidate for candidate in range(1, 2049) if key_count % candidate == 0))


def build_picks(route_rows, experts_count, capacity):
    flat_routes = route_rows.reshape(-1)
    onehot = (flat_routes[:, None] == jnp.arange(experts_count, dtype=jnp.int32)[None, :]).astype(
        jnp.int32
    )
    earlier = jnp.cumsum(onehot, axis=0) - onehot
    slot_rank = jnp.sum(earlier * onehot, axis=1)
    slot_ids = flat_routes * capacity + slot_rank
    picked = slot_ids[:, None] == jnp.arange(experts_count * capacity, dtype=jnp.int32)[None, :]
    return picked.astype(jnp.bfloat16).reshape(
        route_rows.shape[0], route_rows.shape[1], experts_count * capacity
    )


def fill_slots(picked, token_rows):
    occupancy = jnp.sum(picked, axis=1)
    return jnp.einsum(
        "ts,td->sd", occupancy, token_rows, preferred_element_type=jnp.float32
    ).astype(jnp.bfloat16)


MESH_IDS = pl.DeviceIdType.MESH
WHOLE_VMEM = pl.BlockSpec(memory_space=pltpu.VMEM)


def flipped(index, bits):
    result = index
    bit = 1
    while bit <= bits:
        if bits & bit:
            result = result + bit * (1 - 2 * ((index // bit) % 2))
        bit *= 2
    return result


def remote(source, target, send_sem, recv_sem, device):
    return pltpu.make_async_remote_copy(
        src_ref=source,
        dst_ref=target,
        send_sem=send_sem,
        recv_sem=recv_sem,
        device_id=device,
        device_id_type=MESH_IDS,
    )


def greet(devices):
    barrier = pltpu.get_barrier_semaphore()
    for device in devices:
        pl.semaphore_signal(barrier, inc=1, device_id=device, device_id_type=MESH_IDS)
    pl.semaphore_wait(barrier, len(devices))


def sp_peers(members):
    own = lax.axis_index("sp")
    pair, outer = own % 2, own // 2
    partner = {"sp": outer * 2 + 1 - pair}
    others = [{"sp": flipped(outer, d) * 2 + pair} for d in range(1, members // 2)]
    return own, pair, outer, partner, others


def gather_kernel(members, quarters, count, with_tp, *refs):
    x_refs, o_refs = refs[:count], refs[count : 2 * count]
    t_refs = refs[2 * count : 3 * count] if with_tp else ()
    sems = refs[2 * count + len(t_refs) :]
    send_z, recv_z, send_x, recv_x = sems[:4]
    half = members // 2
    own, pair, outer, partner, others = sp_peers(members)
    tp = lax.axis_index("tp")
    mates = [{"tp": flipped(tp, d)} for d in range(1, quarters)] if with_tp else []
    greet([partner] + others + mates)
    to_z = {}
    rest = []
    for i in range(count):
        x_ref, o_ref = x_refs[i], o_refs[i]
        rest.append(remote(x_ref, o_ref.at[own], send_x.at[i, 0], recv_x.at[i, 0], partner))
        for d in range(1, half):
            to_z[d, i] = remote(
                x_ref, o_ref.at[own], send_z.at[i, d], recv_z.at[i, d], others[d - 1]
            )
    for d in range(1, half):
        for i in range(count):
            to_z[d, i].start()
    if with_tp:
        send_t, recv_t = sems[4:]
        for i in range(count):
            for d in range(1, quarters):
                rest.append(
                    remote(
                        x_refs[i],
                        t_refs[i].at[tp],
                        send_t.at[i, d],
                        recv_t.at[i, d],
                        mates[d - 1],
                    )
                )
    for copy in rest:
        copy.start()
    for i in range(count):
        o_refs[i][own] = x_refs[i][...]
        if with_tp:
            t_refs[i][tp] = x_refs[i][...]
    for d in range(1, half):
        block = flipped(outer, d) * 2 + pair
        for i in range(count):
            to_z[d, i].wait_recv()
            held = o_refs[i].at[block]
            copy = remote(held, held, send_x.at[i, d], recv_x.at[i, d], partner)
            copy.start()
            rest.append(copy)
    for copy in rest:
        copy.wait_recv()
    for copy in rest + list(to_z.values()):
        copy.wait_send()


def gather_rows(blocks, collective_id, with_tp):
    members, quarters = lax.axis_size("sp"), lax.axis_size("tp")
    count = len(blocks)
    outs = [jax.ShapeDtypeStruct((members,) + x.shape, x.dtype) for x in blocks]
    sems = [pltpu.SemaphoreType.DMA((count, members // 2))] * 4
    if with_tp:
        outs = outs + [jax.ShapeDtypeStruct((quarters,) + x.shape, x.dtype) for x in blocks]
        sems = sems + [pltpu.SemaphoreType.DMA((count, quarters))] * 2
    return pl.pallas_call(
        functools.partial(gather_kernel, members, quarters, count, with_tp),
        out_shape=tuple(outs),
        in_specs=[WHOLE_VMEM] * count,
        out_specs=tuple([WHOLE_VMEM] * len(outs)),
        scratch_shapes=sems,
        compiler_params=pltpu.CompilerParams(collective_id=collective_id, has_side_effects=True),
        cost_estimate=pl.CostEstimate(flops=0, bytes_accessed=50000000, transcendentals=0),
    )(*blocks)


def attend_group(q_ref, k_ref, v_ref, own_gates_ref, key_gates_ref, head_dim, allowed, out_ref, at):
    heads = q_ref.shape[1] // head_dim
    key_heads = k_ref.shape[1] // head_dim
    for h in range(heads):
        j = h * key_heads // heads
        scores = lax.dot_general(
            q_ref[:, h * head_dim : (h + 1) * head_dim],
            k_ref[:, j * head_dim : (j + 1) * head_dim],
            (((1,), (1,)), ((), ())),
            preferred_element_type=jnp.float32,
        )
        scores = scores * head_dim ** (-0.5) + own_gates_ref[:, h : h + 1] - key_gates_ref[h : h + 1]
        scores = jnp.where(allowed, scores, -1e30)
        weights = jnp.exp(scores - jnp.max(scores, axis=1, keepdims=True))
        weights = jnp.where(allowed, weights, 0.0)
        summed = jnp.dot(
            weights.astype(jnp.bfloat16),
            v_ref[:, j * head_dim : (j + 1) * head_dim],
            preferred_element_type=jnp.float32,
        )
        low = at + h * head_dim
        out_ref[:, low : low + head_dim] = (
            summed / jnp.sum(weights, axis=1, keepdims=True)
        ).astype(jnp.bfloat16)


def attend_kernel(
    fq, fk, fv, fg_own, fg_all, hq, hk, hv, hg_own, hg_all, fo, ho, out_ref, proj, attention, sems
):
    full_width = fo.shape[0]
    loads = [
        pltpu.make_async_copy(fo, proj.at[pl.ds(0, full_width)], sems.at[0]),
        pltpu.make_async_copy(ho, proj.at[pl.ds(full_width, ho.shape[0])], sems.at[1]),
    ]
    for load in loads:
        load.start()
    row_count = fq.shape[0]
    shape = (row_count, fk.shape[0])
    row_pos = lax.axis_index("sp") * row_count + lax.broadcasted_iota(jnp.int32, shape, 0)
    allowed = lax.broadcasted_iota(jnp.int32, shape, 1) <= row_pos
    attend_group(fq, fk, fv, fg_own, fg_all, WD, allowed, attention, 0)
    attend_group(hq, hk, hv, hg_own, hg_all, ND, allowed, attention, full_width)
    for load in loads:
        load.wait()
    step = 512

    @pl.loop(0, out_ref.shape[1] // step)
    def _(c):
        cols = pl.ds(pl.multiple_of(c * step, step), step)
        out_ref[:, cols] = jnp.dot(
            attention[...], proj[:, cols], preferred_element_type=jnp.float32
        ).astype(jnp.bfloat16)


def attend(*arrays):
    row_count = arrays[0].shape[0]
    full_output, half_output = arrays[-2:]
    depth, width = full_output.shape[0] + half_output.shape[0], full_output.shape[1]
    return pl.pallas_call(
        attend_kernel,
        out_shape=jax.ShapeDtypeStruct((row_count, width), jnp.bfloat16),
        in_specs=[WHOLE_VMEM] * (len(arrays) - 2) + [pl.BlockSpec(memory_space=pl.ANY)] * 2,
        out_specs=WHOLE_VMEM,
        scratch_shapes=[
            pltpu.VMEM((depth, width), jnp.bfloat16),
            pltpu.VMEM((row_count, depth), jnp.bfloat16),
            pltpu.SemaphoreType.DMA((2,)),
        ],
        cost_estimate=pl.CostEstimate(flops=0, bytes_accessed=20000000, transcendentals=0),
    )(*arrays)


def hidden_of(rows, weights, unit):
    both = jnp.dot(rows, weights, preferred_element_type=jnp.float32)
    gate_part, up_part = both[:, :unit], both[:, unit:]
    return (gate_part / (1.0 + jnp.exp(-gate_part)) * up_part).astype(jnp.bfloat16)


def hidden_kernel(count, rows_ref, normed_ref, *refs):
    gates, ups = refs[:count], refs[count : 2 * count]
    down_ref, hidden_ref, shared_ref, both, down, sems = refs[2 * count :]
    unit = gates[0].shape[1]
    loads = []
    for b in range(count):
        loads.append(
            (
                pltpu.make_async_copy(gates[b], both.at[b, :, pl.ds(0, unit)], sems.at[b, 0]),
                pltpu.make_async_copy(ups[b], both.at[b, :, pl.ds(unit, unit)], sems.at[b, 1]),
            )
        )
    load_down = pltpu.make_async_copy(down_ref, down, sems.at[count, 0])
    for pair in loads:
        pair[0].start()
        pair[1].start()
    load_down.start()
    for b in range(count):
        loads[b][0].wait()
        loads[b][1].wait()
        if b == 0:
            shared_hidden = hidden_of(normed_ref[...], both[0], unit)
        else:
            hidden_ref[:, (b - 1) * unit : b * unit] = hidden_of(rows_ref[...], both[b], unit)
    load_down.wait()
    step = 512
    for c in range(0, shared_ref.shape[1], step):
        shared_ref[:, c : c + step] = jnp.dot(
            shared_hidden, down[:, c : c + step], preferred_element_type=jnp.float32
        ).astype(jnp.bfloat16)


def hidden_units(rows, normed, gates, ups, shared_down):
    count = len(gates)
    width, unit = gates[0].shape
    return pl.pallas_call(
        functools.partial(hidden_kernel, count),
        out_shape=(
            jax.ShapeDtypeStruct((rows.shape[0], (count - 1) * unit), jnp.bfloat16),
            jax.ShapeDtypeStruct(normed.shape, jnp.bfloat16),
        ),
        in_specs=[WHOLE_VMEM] * 2 + [pl.BlockSpec(memory_space=pl.ANY)] * (2 * count + 1),
        out_specs=(WHOLE_VMEM, WHOLE_VMEM),
        scratch_shapes=[
            pltpu.VMEM((count, width, 2 * unit), jnp.bfloat16),
            pltpu.VMEM(shared_down.shape, jnp.bfloat16),
            pltpu.SemaphoreType.DMA((count + 1, 2)),
        ],
        cost_estimate=pl.CostEstimate(flops=0, bytes_accessed=25000000, transcendentals=0),
    )(rows, normed, *gates, *ups, shared_down)


def down_kernel(count, hidden_ref, scale_ref, *refs):
    downs = refs[:count]
    out_ref, down, sems = refs[count:]
    unit = downs[0].shape[0]
    loads = [
        pltpu.make_async_copy(downs[b], down.at[pl.ds(b * unit, unit)], sems.at[b])
        for b in range(count)
    ]
    for load in loads:
        load.start()
    for load in loads:
        load.wait()
    step = 512

    @pl.loop(0, out_ref.shape[1] // step)
    def _(c):
        cols = pl.ds(pl.multiple_of(c * step, step), step)
        product = jnp.dot(hidden_ref[...], down[:, cols], preferred_element_type=jnp.float32)
        out_ref[:, cols] = (product * scale_ref[...]).astype(jnp.bfloat16)


def down_rows(hidden, scale, downs):
    count = len(downs)
    unit, width = downs[0].shape
    return pl.pallas_call(
        functools.partial(down_kernel, count),
        out_shape=jax.ShapeDtypeStruct((hidden.shape[0], width), jnp.bfloat16),
        in_specs=[WHOLE_VMEM] * 2 + [pl.BlockSpec(memory_space=pl.ANY)] * count,
        out_specs=WHOLE_VMEM,
        scratch_shapes=[
            pltpu.VMEM((count * unit, width), jnp.bfloat16),
            pltpu.SemaphoreType.DMA((count,)),
        ],
        cost_estimate=pl.CostEstimate(flops=0, bytes_accessed=15000000, transcendentals=0),
    )(hidden, scale, *downs)


def add_norm_kernel(
    quarters, parts_ref, residual_ref, gain_ref, middle_ref, normed_ref, landed, send, recv
):
    tp = lax.axis_index("tp")
    mates = [{"tp": flipped(tp, d)} for d in range(1, quarters)]
    greet(mates)
    copies = [
        remote(
            parts_ref.at[flipped(tp, d)], landed.at[d - 1], send.at[d], recv.at[d], mates[d - 1]
        )
        for d in range(1, quarters)
    ]
    for copy in copies:
        copy.start()
    middle = parts_ref[tp].astype(jnp.float32) + residual_ref[...].astype(jnp.float32)
    for d, copy in enumerate(copies):
        copy.wait_recv()
        middle = middle + landed[d].astype(jnp.float32)
    middle_ref[...] = middle
    scale = lax.rsqrt(jnp.mean(middle * middle, axis=-1, keepdims=True) + 1e-06)
    normed_ref[...] = (middle * scale * gain_ref[...]).astype(jnp.bfloat16)
    for copy in copies:
        copy.wait_send()


def add_norm(parts, residual, gain):
    quarters, rows, width = parts.shape
    return pl.pallas_call(
        functools.partial(add_norm_kernel, quarters),
        out_shape=(
            jax.ShapeDtypeStruct((rows, width), jnp.float32),
            jax.ShapeDtypeStruct((rows, width), jnp.bfloat16),
        ),
        in_specs=[WHOLE_VMEM] * 3,
        out_specs=(WHOLE_VMEM, WHOLE_VMEM),
        scratch_shapes=[
            pltpu.VMEM((quarters - 1, rows, width), jnp.bfloat16),
            pltpu.SemaphoreType.DMA((quarters,)),
            pltpu.SemaphoreType.DMA((quarters,)),
        ],
        compiler_params=pltpu.CompilerParams(collective_id=2, has_side_effects=True),
        cost_estimate=pl.CostEstimate(flops=0, bytes_accessed=40000000, transcendentals=0),
    )(parts, residual, gain)


def return_kernel(
    members,
    quarters,
    routed_ref,
    shared_ref,
    middle_ref,
    out_ref,
    from_x,
    staged,
    from_z,
    from_t,
    send_x,
    recv_x,
    send_z,
    recv_z,
    send_t,
    recv_t,
):
    half = members // 2
    own, pair, outer, partner, others = sp_peers(members)
    tp = lax.axis_index("tp")
    mates = [{"tp": flipped(tp, d)} for d in range(1, quarters)]
    greet([partner] + others + mates)
    to_x = [
        remote(
            routed_ref.at[flipped(outer, d) * 2 + 1 - pair],
            from_x.at[d],
            send_x.at[d],
            recv_x.at[d],
            partner,
        )
        for d in range(half)
    ]
    for d in list(range(1, half))[::-1] + [0]:
        to_x[d].start()
    to_t = [
        remote(
            shared_ref.at[flipped(tp, d)], from_t.at[d - 1], send_t.at[d], recv_t.at[d], mates[d - 1]
        )
        for d in range(1, quarters)
    ]
    for copy in to_t:
        copy.start()
    to_z = [
        remote(staged.at[d], from_z.at[d], send_z.at[d], recv_z.at[d], others[d - 1])
        for d in range(1, half)
    ]
    for d in range(1, half)[::-1]:
        to_x[d].wait_recv()
        staged[d] = (
            routed_ref[flipped(outer, d) * 2 + pair].astype(jnp.float32)
            + from_x[d].astype(jnp.float32)
        ).astype(jnp.bfloat16)
        to_z[d - 1].start()
    total = middle_ref[...] + shared_ref[tp].astype(jnp.float32)
    for d, copy in enumerate(to_t):
        copy.wait_recv()
        total = total + from_t[d].astype(jnp.float32)
    to_x[0].wait_recv()
    total = total + routed_ref[own].astype(jnp.float32) + from_x[0].astype(jnp.float32)
    for d in range(1, half):
        to_z[d - 1].wait_recv()
        total = total + from_z[d].astype(jnp.float32)
    out_ref[...] = total.astype(jnp.bfloat16)
    for copy in to_x + to_t + to_z:
        copy.wait_send()


def return_rows(routed, shared, middle):
    members, rows, width = routed.shape
    quarters = shared.shape[0]
    half = members // 2
    sems = [pltpu.SemaphoreType.DMA((half,))] * 4 + [pltpu.SemaphoreType.DMA((quarters,))] * 2
    return pl.pallas_call(
        functools.partial(return_kernel, members, quarters),
        out_shape=jax.ShapeDtypeStruct((rows, width), jnp.bfloat16),
        in_specs=[WHOLE_VMEM] * 3,
        out_specs=WHOLE_VMEM,
        scratch_shapes=[
            pltpu.VMEM((half, rows, width), jnp.bfloat16),
            pltpu.VMEM((half, rows, width), jnp.bfloat16),
            pltpu.VMEM((half, rows, width), jnp.bfloat16),
            pltpu.VMEM((quarters - 1, rows, width), jnp.bfloat16),
        ]
        + sems,
        compiler_params=pltpu.CompilerParams(collective_id=4, has_side_effects=True),
        cost_estimate=pl.CostEstimate(flops=0, bytes_accessed=80000000, transcendentals=0),
    )(routed, shared, middle)


def swapped(arrays, bit):
    pairs = [(j, j ^ bit) for j in range(lax.axis_size("tp"))]
    return [lax.ppermute(array, "tp", pairs) for array in arrays]


def held_until(arrays, other):
    result = lax.optimization_barrier(tuple(arrays) + (other,))
    return list(result[:-1]), result[-1]


def far_blocks(arrays):
    held = list(arrays)
    bit = lax.axis_size("tp") // 2
    while bit > 1:
        held = held + swapped(held, bit)
        bit //= 2
    return held


def body(
    full_queries,
    full_keys,
    full_values,
    full_gates,
    half_queries,
    half_keys,
    half_values,
    half_gates,
    residual,
    full_output,
    half_output,
    norm_gain,
    routes,
    route_weights,
    expert_gate,
    expert_up,
    expert_down,
    shared_gate,
    shared_up,
    shared_down,
):
    row_count = full_queries.shape[0]
    quarters = lax.axis_size("tp")
    quarter = lax.axis_index("tp")
    quarter_rows = row_count // quarters
    experts_count = lax.axis_size("sp")
    own_expert = lax.axis_index("sp")
    capacity = 2 * quarter_rows * TOP // experts_count
    gate_up = far_blocks([expert_gate[0], expert_up[0]])
    offset = own_expert * row_count
    query_pos = offset + jnp.arange(row_count, dtype=jnp.int32)
    dense_routes = capacity >= quarter_rows
    columns = [full_keys, full_values, half_keys, half_values]
    if dense_routes:
        columns = columns + [jnp.transpose(routes), jnp.transpose(route_weights)]
    gathered_rows = gather_rows(columns, 1, False)
    key_count = experts_count * row_count
    members = [rows.reshape(key_count, -1) for rows in gathered_rows[:4]]
    if key_count == span_for(key_count):
        partial_out = attend(
            full_queries,
            members[0],
            members[1],
            lax.dynamic_slice_in_dim(full_gates, offset, row_count, 0),
            jnp.transpose(full_gates),
            half_queries,
            members[2],
            members[3],
            lax.dynamic_slice_in_dim(half_gates, offset, row_count, 0),
            jnp.transpose(half_gates),
            full_output,
            half_output,
        )
    else:
        full_shaped, full_query_gates = group_setup(
            full_queries, full_gates, offset, full_keys.shape[1] // WD, WD
        )
        half_shaped, half_query_gates = group_setup(
            half_queries, half_gates, offset, half_keys.shape[1] // ND, ND
        )
        initial = empty_state(full_shaped) + empty_state(half_shaped)
        span_rows = span_for(key_count)

        def one_span(running, span_index):
            span_start = span_index * span_rows
            sliced = tuple(
                (lax.dynamic_slice_in_dim(member, span_start, span_rows, 0) for member in members)
            )

            def update(current):
                full_new = group_update(
                    current[:3],
                    full_shaped,
                    full_query_gates,
                    full_gates,
                    sliced[0],
                    sliced[1],
                    span_start,
                    query_pos,
                    WD,
                )
                half_new = group_update(
                    current[3:],
                    half_shaped,
                    half_query_gates,
                    half_gates,
                    sliced[2],
                    sliced[3],
                    span_start,
                    query_pos,
                    ND,
                )
                return full_new + half_new

            last_row = offset + row_count - 1
            return (
                lax.cond(span_start <= last_row, update, lambda unchanged: unchanged, running),
                None,
            )

        result, _ = lax.scan(one_span, initial, jnp.arange(key_count // span_rows, dtype=jnp.int32))
        full_attention = group_finish(result[:3])
        half_attention = group_finish(result[3:])
        partial_out = jnp.dot(
            full_attention, full_output, preferred_element_type=jnp.float32
        ) + jnp.dot(half_attention, half_output, preferred_element_type=jnp.float32)
        partial_out = partial_out.astype(jnp.bfloat16)
    gate_up, partial_out = held_until(gate_up, partial_out)
    gate_up = gate_up + swapped(gate_up, 1)
    own_residual = lax.dynamic_slice_in_dim(residual, quarter * quarter_rows, quarter_rows, 0)
    own_middle, own_normed = add_norm(
        partial_out.reshape(quarters, quarter_rows, D),
        own_residual,
        norm_gain.reshape(1, D),
    )
    downs, own_normed = held_until([expert_down[0]], own_normed)
    downs = far_blocks(downs)
    if dense_routes:
        expert_rows, normed = gather_rows([own_normed], 3, True)
        flat_rows = expert_rows.reshape(-1, D)
    else:
        normed = lax.all_gather(own_normed, "tp", axis=0, tiled=True)
        own_routes = lax.dynamic_slice_in_dim(routes, quarter * quarter_rows, quarter_rows, 0)
        own_picks = build_picks(own_routes, experts_count, capacity)
        buffer_rows = fill_slots(own_picks, own_normed).reshape(experts_count, capacity, D)
        received = lax.all_to_all(buffer_rows, "sp", split_axis=0, concat_axis=0, tiled=True)
        flat_rows = received.reshape(-1, D)
    normed = normed.reshape(row_count, D)
    downs, flat_rows = held_until(downs, flat_rows)
    downs = downs + swapped(downs, 1)
    hidden, shared_term = hidden_units(
        flat_rows, normed, [shared_gate] + gate_up[0::2], [shared_up] + gate_up[1::2], shared_down
    )
    shared_term = shared_term.reshape(quarters, quarter_rows, D)
    row_scales = jnp.ones((flat_rows.shape[0], 1), jnp.float32)
    if dense_routes:
        named = jnp.where(gathered_rows[4] == own_expert, gathered_rows[5], 0.0)
        named = jnp.sum(named, axis=1)
        row_scales = lax.dynamic_slice_in_dim(named, quarter * quarter_rows, quarter_rows, 1)
        row_scales = row_scales.reshape(-1, 1)
    routed = down_rows(hidden, row_scales, downs)
    if dense_routes:
        return return_rows(
            routed.reshape(experts_count, quarter_rows, D), shared_term, own_middle
        )
    finished_rows = routed.reshape(received.shape)
    summed = lax.psum_scatter(shared_term, "tp", scatter_dimension=0, tiled=True).astype(
        jnp.float32
    )[0]
    returned = lax.all_to_all(finished_rows, "sp", split_axis=0, concat_axis=0, tiled=True)
    gathered = jnp.einsum(
        "tks,sd->tkd",
        own_picks,
        returned.reshape(experts_count * capacity, D),
        preferred_element_type=jnp.float32,
    )
    own_weights = lax.dynamic_slice_in_dim(route_weights, quarter * quarter_rows, quarter_rows, 0)
    routed = jnp.sum(own_weights[..., None] * gathered, axis=1)
    return (own_middle + summed + routed).astype(jnp.bfloat16)


def solution(mesh):
    return jax.shard_map(
        body,
        mesh=mesh,
        in_specs=(
            P("sp", "tp"),
            P("sp", "tp"),
            P("sp", "tp"),
            P(None, "tp"),
            P("sp", "tp"),
            P("sp", "tp"),
            P("sp", "tp"),
            P(None, "tp"),
            P("sp", None),
            P("tp", None),
            P("tp", None),
            P(),
            P("sp", None),
            P("sp", None),
            P("sp", None, "tp"),
            P("sp", None, "tp"),
            P("sp", "tp", None),
            P(None, "tp"),
            P(None, "tp"),
            P("tp", None),
        ),
        out_specs=P(("sp", "tp"), None),
        check_vma=False,
    )
```

```python
import functools

import jax
import jax.numpy as jnp
from jax import lax
from jax.experimental import pallas as pl
from jax.experimental.pallas import tpu as pltpu
from jax.sharding import PartitionSpec as P

D = 4096
WD = 128
ND = 64
TOP = 4


def group_setup(queries, gates, offset, key_heads, head_dim):
    row_count = queries.shape[0]
    group_size = queries.shape[1] // head_dim // key_heads
    shaped = queries.reshape(row_count, key_heads, group_size, head_dim)
    own_gates = lax.dynamic_slice_in_dim(gates, offset, row_count, 0)
    query_gates = jnp.transpose(own_gates.reshape(row_count, key_heads, group_size), (1, 2, 0))[
        ..., None
    ]
    return (shaped, query_gates)


def empty_state(shaped):
    row_count, key_heads, group_size, head_dim = shaped.shape
    return (
        jnp.full((key_heads, group_size, row_count), -1e30, jnp.float32),
        jnp.zeros((key_heads, group_size, row_count), jnp.float32),
        jnp.zeros((key_heads, group_size, row_count, head_dim), jnp.float32),
    )


def group_update(
    running, shaped, query_gates, all_gates, key_rows, value_rows, span_start, query_pos, head_dim
):
    row_max, row_total, weighted = running
    key_count = key_rows.shape[0]
    key_heads = shaped.shape[1]
    group_size = shaped.shape[2]
    key_shaped = key_rows.reshape(key_count, key_heads, head_dim)
    value_shaped = value_rows.reshape(key_count, key_heads, head_dim)
    key_gates = lax.dynamic_slice_in_dim(all_gates, span_start, key_count, 0)
    key_gates = jnp.transpose(key_gates.reshape(key_count, key_heads, group_size), (1, 2, 0))[
        :, :, None, :
    ]
    scores = jnp.einsum("tkgd,skd->kgts", shaped, key_shaped, preferred_element_type=jnp.float32)
    scores = scores * head_dim ** (-0.5) + query_gates - key_gates
    key_pos = span_start + jnp.arange(key_count, dtype=jnp.int32)
    allowed = key_pos[None, :] <= query_pos[:, None]
    masked = jnp.where(allowed, scores, -1e30)
    new_max = jnp.maximum(row_max, jnp.max(masked, axis=-1))
    weights = jnp.where(allowed, jnp.exp(masked - new_max[..., None]), 0.0)
    shrink = jnp.exp(row_max - new_max)
    new_total = row_total * shrink + jnp.sum(weights, axis=-1)
    new_weighted = weighted * shrink[..., None] + jnp.einsum(
        "kgts,skd->kgtd",
        weights.astype(jnp.bfloat16),
        value_shaped,
        preferred_element_type=jnp.float32,
    )
    return (new_max, new_total, new_weighted)


def group_finish(running):
    weighted = running[2] / running[1][..., None]
    row_count = weighted.shape[2]
    return jnp.transpose(weighted, (2, 0, 1, 3)).reshape(row_count, -1).astype(jnp.bfloat16)


def span_for(key_count):
    if key_count <= 2048:
        return key_count
    return max((candidate for candidate in range(1, 2049) if key_count % candidate == 0))


def build_picks(route_rows, experts_count, capacity):
    flat_routes = route_rows.reshape(-1)
    onehot = (flat_routes[:, None] == jnp.arange(experts_count, dtype=jnp.int32)[None, :]).astype(
        jnp.int32
    )
    earlier = jnp.cumsum(onehot, axis=0) - onehot
    slot_rank = jnp.sum(earlier * onehot, axis=1)
    slot_ids = flat_routes * capacity + slot_rank
    picked = slot_ids[:, None] == jnp.arange(experts_count * capacity, dtype=jnp.int32)[None, :]
    return picked.astype(jnp.bfloat16).reshape(
        route_rows.shape[0], route_rows.shape[1], experts_count * capacity
    )


def fill_slots(picked, token_rows):
    occupancy = jnp.sum(picked, axis=1)
    return jnp.einsum(
        "ts,td->sd", occupancy, token_rows, preferred_element_type=jnp.float32
    ).astype(jnp.bfloat16)


MESH_IDS = pl.DeviceIdType.MESH
WHOLE_VMEM = pl.BlockSpec(memory_space=pltpu.VMEM)
PIECES = 2


def flipped(index, bits):
    result = index
    bit = 1
    while bit <= bits:
        if bits & bit:
            result = result + bit * (1 - 2 * ((index // bit) % 2))
        bit *= 2
    return result


def remote(source, target, send_sem, recv_sem, device):
    return pltpu.make_async_remote_copy(
        src_ref=source,
        dst_ref=target,
        send_sem=send_sem,
        recv_sem=recv_sem,
        device_id=device,
        device_id_type=MESH_IDS,
    )


def greet(devices):
    barrier = pltpu.get_barrier_semaphore()
    for device in devices:
        pl.semaphore_signal(barrier, inc=1, device_id=device, device_id_type=MESH_IDS)
    pl.semaphore_wait(barrier, len(devices))


def sp_peers(members):
    own = lax.axis_index("sp")
    pair, outer = own % 2, own // 2
    partner = {"sp": outer * 2 + 1 - pair}
    others = [{"sp": flipped(outer, d) * 2 + pair} for d in range(1, members // 2)]
    return own, pair, outer, partner, others


def gather_kernel(members, quarters, count, with_tp, *refs):
    x_refs, o_refs = refs[:count], refs[count : 2 * count]
    t_refs = refs[2 * count : 3 * count] if with_tp else ()
    sems = refs[2 * count + len(t_refs) :]
    send_z, recv_z, send_x, recv_x = sems[:4]
    half = members // 2
    own, pair, outer, partner, others = sp_peers(members)
    tp = lax.axis_index("tp")
    mates = [{"tp": flipped(tp, d)} for d in range(1, quarters)] if with_tp else []
    greet([partner] + others + mates)
    to_z = {}
    rest = []
    for i in range(count):
        x_ref, o_ref = x_refs[i], o_refs[i]
        rest.append(remote(x_ref, o_ref.at[own], send_x.at[i, 0], recv_x.at[i, 0], partner))
        for d in range(1, half):
            to_z[d, i] = remote(
                x_ref, o_ref.at[own], send_z.at[i, d], recv_z.at[i, d], others[d - 1]
            )
    for d in range(1, half):
        for i in range(count):
            to_z[d, i].start()
    if with_tp:
        send_t, recv_t = sems[4:]
        for i in range(count):
            for d in range(1, quarters):
                rest.append(
                    remote(
                        x_refs[i],
                        t_refs[i].at[tp],
                        send_t.at[i, d],
                        recv_t.at[i, d],
                        mates[d - 1],
                    )
                )
    for copy in rest:
        copy.start()
    for i in range(count):
        o_refs[i][own] = x_refs[i][...]
        if with_tp:
            t_refs[i][tp] = x_refs[i][...]
    for d in range(1, half):
        block = flipped(outer, d) * 2 + pair
        for i in range(count):
            to_z[d, i].wait_recv()
            held = o_refs[i].at[block]
            copy = remote(held, held, send_x.at[i, d], recv_x.at[i, d], partner)
            copy.start()
            rest.append(copy)
    for copy in rest:
        copy.wait_recv()
    for copy in rest + list(to_z.values()):
        copy.wait_send()


def gather_rows(blocks, collective_id, with_tp):
    members, quarters = lax.axis_size("sp"), lax.axis_size("tp")
    count = len(blocks)
    outs = [jax.ShapeDtypeStruct((members,) + x.shape, x.dtype) for x in blocks]
    sems = [pltpu.SemaphoreType.DMA((count, members // 2))] * 4
    if with_tp:
        outs = outs + [jax.ShapeDtypeStruct((quarters,) + x.shape, x.dtype) for x in blocks]
        sems = sems + [pltpu.SemaphoreType.DMA((count, quarters))] * 2
    return pl.pallas_call(
        functools.partial(gather_kernel, members, quarters, count, with_tp),
        out_shape=tuple(outs),
        in_specs=[WHOLE_VMEM] * count,
        out_specs=tuple([WHOLE_VMEM] * len(outs)),
        scratch_shapes=sems,
        compiler_params=pltpu.CompilerParams(collective_id=collective_id, has_side_effects=True),
        cost_estimate=pl.CostEstimate(flops=0, bytes_accessed=50000000, transcendentals=0),
    )(*blocks)


def attend_group(q_ref, k_ref, v_ref, own_gates_ref, key_gates_ref, head_dim, allowed, out_ref, at):
    heads = q_ref.shape[1] // head_dim
    key_heads = k_ref.shape[1] // head_dim
    for h in range(heads):
        j = h * key_heads // heads
        scores = lax.dot_general(
            q_ref[:, h * head_dim : (h + 1) * head_dim],
            k_ref[:, j * head_dim : (j + 1) * head_dim],
            (((1,), (1,)), ((), ())),
            preferred_element_type=jnp.float32,
        )
        scores = scores * head_dim ** (-0.5) + own_gates_ref[:, h : h + 1] - key_gates_ref[h : h + 1]
        scores = jnp.where(allowed, scores, -1e30)
        weights = jnp.exp(scores - jnp.max(scores, axis=1, keepdims=True))
        weights = jnp.where(allowed, weights, 0.0)
        summed = jnp.dot(
            weights.astype(jnp.bfloat16),
            v_ref[:, j * head_dim : (j + 1) * head_dim],
            preferred_element_type=jnp.float32,
        )
        low = at + h * head_dim
        out_ref[:, low : low + head_dim] = (
            summed / jnp.sum(weights, axis=1, keepdims=True)
        ).astype(jnp.bfloat16)


def attend_kernel(
    fq, fk, fv, fg_own, fg_all, hq, hk, hv, hg_own, hg_all, fo, ho, out_ref, proj, attention, sems
):
    full_width = fo.shape[0]
    loads = [
        pltpu.make_async_copy(fo, proj.at[pl.ds(0, full_width)], sems.at[0]),
        pltpu.make_async_copy(ho, proj.at[pl.ds(full_width, ho.shape[0])], sems.at[1]),
    ]
    for load in loads:
        load.start()
    row_count = fq.shape[0]
    shape = (row_count, fk.shape[0])
    row_pos = lax.axis_index("sp") * row_count + lax.broadcasted_iota(jnp.int32, shape, 0)
    allowed = lax.broadcasted_iota(jnp.int32, shape, 1) <= row_pos
    attend_group(fq, fk, fv, fg_own, fg_all, WD, allowed, attention, 0)
    attend_group(hq, hk, hv, hg_own, hg_all, ND, allowed, attention, full_width)
    for load in loads:
        load.wait()
    step = 512

    @pl.loop(0, out_ref.shape[1] // step)
    def _(c):
        cols = pl.ds(pl.multiple_of(c * step, step), step)
        out_ref[:, cols] = jnp.dot(
            attention[...], proj[:, cols], preferred_element_type=jnp.float32
        ).astype(jnp.bfloat16)


def attend(*arrays):
    row_count = arrays[0].shape[0]
    full_output, half_output = arrays[-2:]
    depth, width = full_output.shape[0] + half_output.shape[0], full_output.shape[1]
    return pl.pallas_call(
        attend_kernel,
        out_shape=jax.ShapeDtypeStruct((row_count, width), jnp.bfloat16),
        in_specs=[WHOLE_VMEM] * (len(arrays) - 2) + [pl.BlockSpec(memory_space=pl.ANY)] * 2,
        out_specs=WHOLE_VMEM,
        scratch_shapes=[
            pltpu.VMEM((depth, width), jnp.bfloat16),
            pltpu.VMEM((row_count, depth), jnp.bfloat16),
            pltpu.SemaphoreType.DMA((2,)),
        ],
        cost_estimate=pl.CostEstimate(flops=0, bytes_accessed=20000000, transcendentals=0),
    )(*arrays)


def hidden_of(rows, weights, unit):
    split = rows[0].shape[1]
    both = jnp.dot(rows[0][...], weights[:split], preferred_element_type=jnp.float32)
    both = both + jnp.dot(rows[1][...], weights[split:], preferred_element_type=jnp.float32)
    gate_part, up_part = both[:, :unit], both[:, unit:]
    return (gate_part / (1.0 + jnp.exp(-gate_part)) * up_part).astype(jnp.bfloat16)


def hidden_kernel(count, *refs):
    rows, normed = refs[:2], refs[2:4]
    gates, lows, highs = (refs[4 + i * count : 4 + (i + 1) * count] for i in range(3))
    down_ref, hidden_ref, shared_ref, both, down, sems = refs[4 + 3 * count :]
    split = lows[0].shape[0]
    unit = gates[0].shape[1]
    loads = []
    for b in range(count):
        loads.append(
            (
                pltpu.make_async_copy(gates[b], both.at[b, :, pl.ds(0, unit)], sems.at[b, 0]),
                pltpu.make_async_copy(
                    lows[b], both.at[b, pl.ds(0, split), pl.ds(unit, unit)], sems.at[b, 1]
                ),
                pltpu.make_async_copy(
                    highs[b], both.at[b, pl.ds(split, split), pl.ds(unit, unit)], sems.at[b, 2]
                ),
            )
        )
    load_down = pltpu.make_async_copy(down_ref, down, sems.at[count, 0])
    for three in loads:
        for load in three:
            load.start()
    load_down.start()
    for b in range(count):
        for load in loads[b]:
            load.wait()
        if b == 0:
            shared_hidden = hidden_of(normed, both.at[0], unit)
        else:
            hidden_ref[:, (b - 1) * unit : b * unit] = hidden_of(rows, both.at[b], unit)
    load_down.wait()
    step = 512
    for c in range(0, shared_ref.shape[1], step):
        shared_ref[:, c : c + step] = jnp.dot(
            shared_hidden, down[:, c : c + step], preferred_element_type=jnp.float32
        ).astype(jnp.bfloat16)


def hidden_units(rows, normed, gates, lows, highs, shared_down):
    count = len(gates)
    width, unit = gates[0].shape
    return pl.pallas_call(
        functools.partial(hidden_kernel, count),
        out_shape=(
            jax.ShapeDtypeStruct((rows[0].shape[0], (count - 1) * unit), jnp.bfloat16),
            jax.ShapeDtypeStruct((normed[0].shape[0], width), jnp.bfloat16),
        ),
        in_specs=[WHOLE_VMEM] * 4 + [pl.BlockSpec(memory_space=pl.ANY)] * (3 * count + 1),
        out_specs=(WHOLE_VMEM, WHOLE_VMEM),
        scratch_shapes=[
            pltpu.VMEM((count, width, 2 * unit), jnp.bfloat16),
            pltpu.VMEM(shared_down.shape, jnp.bfloat16),
            pltpu.SemaphoreType.DMA((count + 1, 3)),
        ],
        cost_estimate=pl.CostEstimate(flops=0, bytes_accessed=25000000, transcendentals=0),
    )(*rows, *normed, *gates, *lows, *highs, shared_down)


def down_kernel(count, hidden_ref, scale_ref, *refs):
    downs = refs[:count]
    out_ref, down, sems = refs[count:]
    unit = downs[0].shape[0]
    loads = [
        pltpu.make_async_copy(downs[b], down.at[pl.ds(b * unit, unit)], sems.at[b])
        for b in range(count)
    ]
    for load in loads:
        load.start()
    for load in loads:
        load.wait()
    step = 512

    @pl.loop(0, out_ref.shape[1] // step)
    def _(c):
        cols = pl.ds(pl.multiple_of(c * step, step), step)
        product = jnp.dot(hidden_ref[...], down[:, cols], preferred_element_type=jnp.float32)
        out_ref[:, cols] = (product * scale_ref[...]).astype(jnp.bfloat16)


def down_rows(hidden, scale, downs):
    count = len(downs)
    unit, width = downs[0].shape
    return pl.pallas_call(
        functools.partial(down_kernel, count),
        out_shape=jax.ShapeDtypeStruct((hidden.shape[0], width), jnp.bfloat16),
        in_specs=[WHOLE_VMEM] * 2 + [pl.BlockSpec(memory_space=pl.ANY)] * count,
        out_specs=WHOLE_VMEM,
        scratch_shapes=[
            pltpu.VMEM((count * unit, width), jnp.bfloat16),
            pltpu.SemaphoreType.DMA((count,)),
        ],
        cost_estimate=pl.CostEstimate(flops=0, bytes_accessed=15000000, transcendentals=0),
    )(hidden, scale, *downs)


def add_norm_kernel(
    quarters, parts_ref, residual_ref, gain_ref, middle_ref, low_ref, high_ref, landed, send, recv
):
    tp = lax.axis_index("tp")
    mates = [{"tp": flipped(tp, d)} for d in range(1, quarters)]
    greet(mates)
    copies = [
        remote(
            parts_ref.at[flipped(tp, d)], landed.at[d - 1], send.at[d], recv.at[d], mates[d - 1]
        )
        for d in range(1, quarters)
    ]
    for copy in copies:
        copy.start()
    middle = parts_ref[tp].astype(jnp.float32) + residual_ref[...].astype(jnp.float32)
    for d, copy in enumerate(copies):
        copy.wait_recv()
        middle = middle + landed[d].astype(jnp.float32)
    middle_ref[...] = middle
    scale = lax.rsqrt(jnp.mean(middle * middle, axis=-1, keepdims=True) + 1e-06)
    normed = (middle * scale * gain_ref[...]).astype(jnp.bfloat16)
    low_ref[...] = normed[:, : low_ref.shape[1]]
    high_ref[...] = normed[:, low_ref.shape[1] :]
    for copy in copies:
        copy.wait_send()


def add_norm(parts, residual, gain):
    quarters, rows, width = parts.shape
    return pl.pallas_call(
        functools.partial(add_norm_kernel, quarters),
        out_shape=(
            jax.ShapeDtypeStruct((rows, width), jnp.float32),
            jax.ShapeDtypeStruct((rows, width // 2), jnp.bfloat16),
            jax.ShapeDtypeStruct((rows, width // 2), jnp.bfloat16),
        ),
        in_specs=[WHOLE_VMEM] * 3,
        out_specs=(WHOLE_VMEM, WHOLE_VMEM, WHOLE_VMEM),
        scratch_shapes=[
            pltpu.VMEM((quarters - 1, rows, width), jnp.bfloat16),
            pltpu.SemaphoreType.DMA((quarters,)),
            pltpu.SemaphoreType.DMA((quarters,)),
        ],
        compiler_params=pltpu.CompilerParams(collective_id=2, has_side_effects=True),
        cost_estimate=pl.CostEstimate(flops=0, bytes_accessed=40000000, transcendentals=0),
    )(parts, residual, gain)


def return_kernel(
    members,
    quarters,
    routed_ref,
    shared_ref,
    middle_ref,
    out_ref,
    from_x,
    staged,
    from_z,
    from_t,
    send_x,
    recv_x,
    send_z,
    recv_z,
    send_t,
    recv_t,
):
    half = members // 2
    own, pair, outer, partner, others = sp_peers(members)
    tp = lax.axis_index("tp")
    mates = [{"tp": flipped(tp, d)} for d in range(1, quarters)]
    greet([partner] + others + mates)
    span = routed_ref.shape[2] // PIECES
    pieces = [pl.ds(c * span, span) for c in range(PIECES)]
    far_first = list(range(1, half))[::-1]
    to_x, to_z, to_t = {}, {}, {}
    for d in far_first + [0]:
        for c, cols in enumerate(pieces):
            to_x[d, c] = remote(
                routed_ref.at[flipped(outer, d) * 2 + 1 - pair, :, cols],
                from_x.at[d, :, cols],
                send_x.at[d, c],
                recv_x.at[d, c],
                partner,
            )
            to_x[d, c].start()
    for d in range(1, quarters):
        to_t[d] = remote(
            shared_ref.at[flipped(tp, d)], from_t.at[d - 1], send_t.at[d], recv_t.at[d], mates[d - 1]
        )
        to_t[d].start()
    for d in far_first:
        for c, cols in enumerate(pieces):
            to_x[d, c].wait_recv()
            staged[d, :, cols] = (
                routed_ref[flipped(outer, d) * 2 + pair, :, cols].astype(jnp.float32)
                + from_x[d, :, cols].astype(jnp.float32)
            ).astype(jnp.bfloat16)
            to_z[d, c] = remote(
                staged.at[d, :, cols],
                from_z.at[d, :, cols],
                send_z.at[d, c],
                recv_z.at[d, c],
                others[d - 1],
            )
            to_z[d, c].start()
    for copy in to_t.values():
        copy.wait_recv()
    for c, cols in enumerate(pieces):
        total = middle_ref[:, cols] + shared_ref[tp, :, cols].astype(jnp.float32)
        for d in range(1, quarters):
            total = total + from_t[d - 1, :, cols].astype(jnp.float32)
        to_x[0, c].wait_recv()
        total = total + routed_ref[own, :, cols].astype(jnp.float32)
        total = total + from_x[0, :, cols].astype(jnp.float32)
        for d in far_first:
            to_z[d, c].wait_recv()
            total = total + from_z[d, :, cols].astype(jnp.float32)
        out_ref[:, cols] = total.astype(jnp.bfloat16)
    for copy in list(to_x.values()) + list(to_t.values()) + list(to_z.values()):
        copy.wait_send()


def return_rows(routed, shared, middle):
    members, rows, width = routed.shape
    quarters = shared.shape[0]
    half = members // 2
    sems = [pltpu.SemaphoreType.DMA((half, PIECES))] * 4
    sems = sems + [pltpu.SemaphoreType.DMA((quarters,))] * 2
    return pl.pallas_call(
        functools.partial(return_kernel, members, quarters),
        out_shape=jax.ShapeDtypeStruct((rows, width), jnp.bfloat16),
        in_specs=[WHOLE_VMEM] * 3,
        out_specs=WHOLE_VMEM,
        scratch_shapes=[
            pltpu.VMEM((half, rows, width), jnp.bfloat16),
            pltpu.VMEM((half, rows, width), jnp.bfloat16),
            pltpu.VMEM((half, rows, width), jnp.bfloat16),
            pltpu.VMEM((quarters - 1, rows, width), jnp.bfloat16),
        ]
        + sems,
        compiler_params=pltpu.CompilerParams(collective_id=4, has_side_effects=True),
        cost_estimate=pl.CostEstimate(flops=0, bytes_accessed=80000000, transcendentals=0),
    )(routed, shared, middle)


def swapped(arrays, bit):
    pairs = [(j, j ^ bit) for j in range(lax.axis_size("tp"))]
    return [lax.ppermute(array, "tp", pairs) for array in arrays]


def held_until(arrays, other):
    result = lax.optimization_barrier(tuple(arrays) + (other,))
    return list(result[:-1]), result[-1]


def far_blocks(arrays):
    held = list(arrays)
    bit = lax.axis_size("tp") // 2
    while bit > 1:
        held = held + swapped(held, bit)
        bit //= 2
    return held


def body(
    full_queries,
    full_keys,
    full_values,
    full_gates,
    half_queries,
    half_keys,
    half_values,
    half_gates,
    residual,
    full_output,
    half_output,
    norm_gain,
    routes,
    route_weights,
    expert_gate,
    expert_up,
    expert_down,
    shared_gate,
    shared_up,
    shared_down,
):
    row_count = full_queries.shape[0]
    quarters = lax.axis_size("tp")
    quarter = lax.axis_index("tp")
    quarter_rows = row_count // quarters
    experts_count = lax.axis_size("sp")
    own_expert = lax.axis_index("sp")
    capacity = 2 * quarter_rows * TOP // experts_count
    split = expert_up.shape[1] // 2
    early = [expert_gate[0], expert_up[0, :split]]
    late = [expert_up[0, split:], expert_down[0]]
    near_early, near_late = swapped(early, 1), swapped(late, 1)
    far_early = far_blocks(early)[2:]
    offset = own_expert * row_count
    query_pos = offset + jnp.arange(row_count, dtype=jnp.int32)
    dense_routes = capacity >= quarter_rows
    columns = [full_keys, full_values, half_keys, half_values]
    if dense_routes:
        columns = columns + [jnp.transpose(routes), jnp.transpose(route_weights)]
    gathered_rows = gather_rows(columns, 1, False)
    key_count = experts_count * row_count
    members = [rows.reshape(key_count, -1) for rows in gathered_rows[:4]]
    if key_count == span_for(key_count):
        partial_out = attend(
            full_queries,
            members[0],
            members[1],
            lax.dynamic_slice_in_dim(full_gates, offset, row_count, 0),
            jnp.transpose(full_gates),
            half_queries,
            members[2],
            members[3],
            lax.dynamic_slice_in_dim(half_gates, offset, row_count, 0),
            jnp.transpose(half_gates),
            full_output,
            half_output,
        )
    else:
        full_shaped, full_query_gates = group_setup(
            full_queries, full_gates, offset, full_keys.shape[1] // WD, WD
        )
        half_shaped, half_query_gates = group_setup(
            half_queries, half_gates, offset, half_keys.shape[1] // ND, ND
        )
        initial = empty_state(full_shaped) + empty_state(half_shaped)
        span_rows = span_for(key_count)

        def one_span(running, span_index):
            span_start = span_index * span_rows
            sliced = tuple(
                (lax.dynamic_slice_in_dim(member, span_start, span_rows, 0) for member in members)
            )

            def update(current):
                full_new = group_update(
                    current[:3],
                    full_shaped,
                    full_query_gates,
                    full_gates,
                    sliced[0],
                    sliced[1],
                    span_start,
                    query_pos,
                    WD,
                )
                half_new = group_update(
                    current[3:],
                    half_shaped,
                    half_query_gates,
                    half_gates,
                    sliced[2],
                    sliced[3],
                    span_start,
                    query_pos,
                    ND,
                )
                return full_new + half_new

            last_row = offset + row_count - 1
            return (
                lax.cond(span_start <= last_row, update, lambda unchanged: unchanged, running),
                None,
            )

        result, _ = lax.scan(one_span, initial, jnp.arange(key_count // span_rows, dtype=jnp.int32))
        full_attention = group_finish(result[:3])
        half_attention = group_finish(result[3:])
        partial_out = jnp.dot(
            full_attention, full_output, preferred_element_type=jnp.float32
        ) + jnp.dot(half_attention, half_output, preferred_element_type=jnp.float32)
        partial_out = partial_out.astype(jnp.bfloat16)
    far_early, partial_out = held_until(far_early, partial_out)
    early = early + near_early + far_early + swapped(far_early, 1)
    own_residual = lax.dynamic_slice_in_dim(residual, quarter * quarter_rows, quarter_rows, 0)
    own_middle, own_low, own_high = add_norm(
        partial_out.reshape(quarters, quarter_rows, D),
        own_residual,
        norm_gain.reshape(1, D),
    )
    sources, own_low = held_until(late, own_low)
    far_late = far_blocks(sources)[2:]
    if dense_routes:
        halves = gather_rows([own_low, own_high], 3, True)
        flat_rows = [rows.reshape(-1, D // 2) for rows in halves[:2]]
        normed = [rows.reshape(-1, D // 2) for rows in halves[2:]]
    else:
        own_normed = jnp.concatenate([own_low, own_high], axis=1)
        normed = lax.all_gather(own_normed, "tp", axis=0, tiled=True)
        normed = [normed[:, : D // 2], normed[:, D // 2 :]]
        own_routes = lax.dynamic_slice_in_dim(routes, quarter * quarter_rows, quarter_rows, 0)
        own_picks = build_picks(own_routes, experts_count, capacity)
        buffer_rows = fill_slots(own_picks, own_normed).reshape(experts_count, capacity, D)
        received = lax.all_to_all(buffer_rows, "sp", split_axis=0, concat_axis=0, tiled=True)
        received_rows = received.reshape(-1, D)
        flat_rows = [received_rows[:, : D // 2], received_rows[:, D // 2 :]]
    far_high, flat_rows[0] = held_until(far_late[0::2], flat_rows[0])
    highs = [late[0], near_late[0]] + far_high + swapped(far_high, 1)
    hidden, shared_term = hidden_units(
        flat_rows,
        normed,
        [shared_gate] + early[0::2],
        [shared_up[:split]] + early[1::2],
        [shared_up[split:]] + highs,
        shared_down,
    )
    far_down, hidden = held_until(far_late[1::2], hidden)
    downs = [late[1], near_late[1]] + far_down + swapped(far_down, 1)
    shared_term = shared_term.reshape(quarters, quarter_rows, D)
    row_scales = jnp.ones((flat_rows[0].shape[0], 1), jnp.float32)
    if dense_routes:
        named = jnp.where(gathered_rows[4] == own_expert, gathered_rows[5], 0.0)
        named = jnp.sum(named, axis=1)
        row_scales = lax.dynamic_slice_in_dim(named, quarter * quarter_rows, quarter_rows, 1)
        row_scales = row_scales.reshape(-1, 1)
    routed = down_rows(hidden, row_scales, downs)
    if dense_routes:
        return return_rows(
            routed.reshape(experts_count, quarter_rows, D), shared_term, own_middle
        )
    finished_rows = routed.reshape(received.shape)
    summed = lax.psum_scatter(shared_term, "tp", scatter_dimension=0, tiled=True).astype(
        jnp.float32
    )[0]
    returned = lax.all_to_all(finished_rows, "sp", split_axis=0, concat_axis=0, tiled=True)
    gathered = jnp.einsum(
        "tks,sd->tkd",
        own_picks,
        returned.reshape(experts_count * capacity, D),
        preferred_element_type=jnp.float32,
    )
    own_weights = lax.dynamic_slice_in_dim(route_weights, quarter * quarter_rows, quarter_rows, 0)
    routed = jnp.sum(own_weights[..., None] * gathered, axis=1)
    return (own_middle + summed + routed).astype(jnp.bfloat16)


def solution(mesh):
    return jax.shard_map(
        body,
        mesh=mesh,
        in_specs=(
            P("sp", "tp"),
            P("sp", "tp"),
            P("sp", "tp"),
            P(None, "tp"),
            P("sp", "tp"),
            P("sp", "tp"),
            P("sp", "tp"),
            P(None, "tp"),
            P("sp", None),
            P("tp", None),
            P("tp", None),
            P(),
            P("sp", None),
            P("sp", None),
            P("sp", None, "tp"),
            P("sp", None, "tp"),
            P("sp", "tp", None),
            P(None, "tp"),
            P(None, "tp"),
            P("tp", None),
        ),
        out_specs=P(("sp", "tp"), None),
        check_vma=False,
    )
```
